32 devices in a mesh: sp: 16 (over z, x, core), tp: 2 (over y).
Axes of the slice: x: 2, y: 2, z: 4, core: 2. Of those that a mesh axis runs over, the one named last changes fastest.
Arguments:
- stream: bfloat16 [6144, 2048], P(('sp', 'tp')), may hold values from -6 to 6
- query_narrow: bfloat16 [6144, 512], P('sp', 'tp'), may hold values from -6 to 6
- key_narrow: bfloat16 [6144, 512], P('sp', 'tp'), may hold values from -6.5 to 6.5
- query_wide: bfloat16 [6144, 1024], P('sp', 'tp'), may hold values from -6 to 6
- key_wide: bfloat16 [6144, 1024], P('sp', 'tp'), may hold values from -6.5 to 6.5
- values: bfloat16 [6144, 2, 1024], P('sp', None, 'tp'), may hold values from -6 to 6
- out_gate: bfloat16 [6144, 2, 1024], P('sp', None, 'tp'), may hold values from -6 to 6
- out_weight: bfloat16 [2, 1024, 2048], P(None, 'tp'), may hold values from -0.125 to 0.125
- norm_gain: float32 [2048], replicated, may hold values from 0.1 to 1.9
- mlp_gate: bfloat16 [2048, 5632], P('sp', 'tp'), may hold values from -0.125 to 0.125
- mlp_up: bfloat16 [2048, 5632], P('sp', 'tp'), may hold values from -0.125 to 0.125
- mlp_down: bfloat16 [5632, 2048], P('tp', 'sp'), may hold values from -0.15625 to 0.15625
- log_decay: float32 [2, 2, 8], P(None, None, 'tp'), as said below
Outputs:
- layer_out: bfloat16 [6144, 2048], P(('sp', 'tp'))
The draws below stay inside these ranges and needn't reach their ends.
Inputs may be any that keep to these rules, and one draw needn't show every extreme that they name: `log_decay`: every entry is negative, with magnitude at least 0.5 / 6144.
All inputs are finite; a program needn't handle non-finite values.
Results may differ from the reference program's by a relative error of at most 0.013.
Values may be sent and summed in bfloat16 or wider, within the bound.
A program may use at most 128 MiB of HBM per device.

```python
import jax
import jax.numpy as jnp
from jax import lax

D = 2048
FF = 5632
HG = 8
KA = 64
KB = 128
DV = 128
BLOCK = 128
TOK_DEV = 384
TOKENS = 6144
N_SP = 16


def draw_log_decay(key, part):
    slow_rates = jnp.exp(jax.random.uniform(jax.random.fold_in(key, 11), (2, 2, HG), jnp.float32, jnp.log(0.5), jnp.log(2.3))) / TOKENS
    fast_rates = jnp.exp(jax.random.uniform(jax.random.fold_in(key, 12), (2, 2, HG), jnp.float32, jnp.log(0.01), jnp.log(1.0 / 30.0)))
    forward_rank = jax.random.permutation(jax.random.fold_in(key, 13), 2 * HG)
    backward_rank = jax.random.permutation(jax.random.fold_in(key, 14), 2 * HG)
    ranking = jnp.stack([forward_rank, backward_rank]).reshape(2, 2, HG)
    chosen = jnp.where(ranking < HG, fast_rates, slow_rates)
    return -chosen


def steady_keys(key, head_size):
    result = jnp.clip(jax.random.normal(jax.random.fold_in(key, 1), (TOKENS, HG, head_size), jnp.float32), -6.0, 6.0)
    return result.reshape(TOKENS, HG * head_size).astype(jnp.bfloat16)


def draw_key_narrow(key, part):
    return steady_keys(jax.random.fold_in(key, 21), KA)


def draw_key_wide(key, part):
    return steady_keys(jax.random.fold_in(key, 31), KB)


def draw_values(key, part):
    base_key = jax.random.fold_in(key, 41)
    result = jnp.clip(jax.random.normal(jax.random.fold_in(base_key, 1), (TOKENS, 2, HG * DV), jnp.float32), -6.0, 6.0)
    return result.astype(jnp.bfloat16)


def steps_of(stream_key, dims, shards, low, high):
    factor_of, own = 1.0, jax.random.fold_in(stream_key, 6)
    for axis_at, parts in shards:
        steps = jnp.exp(jax.random.uniform(jax.random.fold_in(own, axis_at), (parts,), jnp.float32, low / len(shards), high / len(shards)))
        factor_of = factor_of * jnp.repeat(steps, dims[axis_at] // parts).reshape([-1 if axis == axis_at else 1 for axis in range(len(dims))])
    return factor_of


def normal_values(key, dims, spread, reach, cuts=(), kind=jnp.bfloat16):
    entries = jax.random.normal(key, dims, jnp.float32) * spread
    if len(cuts) > 0:
        entries = steps_of(key, dims, cuts, -0.22, 0.18) * entries
    return jnp.clip(entries, min=-reach, max=reach).astype(kind)


def setup_inputs(seed: int = 0) -> dict:
    keys = jax.random.split(jax.random.key(seed), 14)
    return {
        "stream": normal_values(keys[0], (TOKENS, D), 1.0, 6.0, ((0, 32),)),
        "query_narrow": normal_values(keys[1], (TOKENS, HG * KA), 1.0, 6.0, ((0, 16), (1, 2))),
        "key_narrow": draw_key_narrow(jax.random.fold_in(keys[13], 71), 0),
        "query_wide": normal_values(keys[3], (TOKENS, HG * KB), 1.0, 6.0, ((0, 16), (1, 2))),
        "key_wide": draw_key_wide(jax.random.fold_in(keys[13], 71), 0),
        "values": draw_values(jax.random.fold_in(keys[13], 71), 0),
        "out_gate": normal_values(keys[6], (TOKENS, 2, HG * DV), 1.0, 6.0, ((0, 16), (2, 2))),
        "out_weight": normal_values(keys[7], (2, HG * DV, D), (2 * HG * DV) ** -0.5, 0.125, ((1, 2),)),
        "norm_gain": jnp.clip(1.0 + 0.18 * jax.random.normal(keys[8], (D,), jnp.float32), 0.1, 1.9),
        "mlp_gate": normal_values(keys[9], (D, FF), D ** -0.5, 0.125, ((0, 16), (1, 2))),
        "mlp_up": normal_values(keys[10], (D, FF), D ** -0.5, 0.125, ((0, 16), (1, 2))),
        "mlp_down": normal_values(keys[11], (FF, D), (FF // 4) ** -0.5, 0.15625, ((0, 2), (1, 16))),
        "log_decay": draw_log_decay(jax.random.fold_in(keys[13], 71), 0),
    }


NORM_EPSILON = 1e-06
ROPE_BASE = 10000.0

def rotate(block_in, positions):
    half_size = block_in.shape[-1] // 2
    frequencies = jnp.power(ROPE_BASE, -(jnp.arange(half_size, dtype=jnp.float32) / half_size))
    angles = positions[:, None] * frequencies[None, :]
    cosine = jnp.cos(angles)[:, None, :]
    sine_table = jnp.sin(angles)[:, None, :]
    first_half = block_in[..., :half_size]
    second_half = block_in[..., half_size:]
    return jnp.concatenate([first_half * cosine - second_half * sine_table, first_half * sine_table + second_half * cosine], -1)

def decay_tables(rate_fwd, rate_bwd, block_len):
    position = jnp.arange(block_len, dtype=jnp.float32)
    offset = position[:, None] - position[None, :]
    forward_part = jnp.exp(rate_fwd[:, None, None] * jnp.maximum(offset, 0.0)[None])
    backward_part = jnp.exp(rate_bwd[:, None, None] * jnp.maximum(-offset, 0.0)[None])
    inner = jnp.where(offset[None] > 0, forward_part, jnp.where(offset[None] < 0, backward_part, 2.0))
    keep_fwd = jnp.exp(rate_fwd[:, None] * (block_len - 1.0 - position)[None, :])
    keep_bwd = jnp.exp(rate_bwd[:, None] * position[None, :])
    reach_fwd = jnp.exp(rate_fwd[:, None] * (position + 1.0)[None, :])
    reach_bwd = jnp.exp(rate_bwd[:, None] * (block_len - position)[None, :])
    return (inner, keep_fwd, keep_bwd, reach_fwd, reach_bwd)

def head_gate(combined, gate_rows):
    mean_value = lax.optimization_barrier(jnp.mean(combined, -1, keepdims=True))
    centred = combined - mean_value
    variance = lax.optimization_barrier(jnp.mean(centred * centred, -1, keepdims=True))
    scaled = centred * lax.rsqrt(variance + NORM_EPSILON)
    gated = jax.nn.silu(gate_rows.astype(jnp.float32)).reshape(combined.shape) * scaled
    return gated.reshape(combined.shape[0], -1).astype(jnp.bfloat16)

def retention_group(query_rows, key_rows, value_rows, gate_rows, rate_fwd, rate_bwd):
    length = query_rows.shape[0]
    head_count = rate_fwd.shape[0]
    key_size = query_rows.shape[1] // head_count
    value_size = value_rows.shape[1] // head_count
    positions = jnp.arange(length, dtype=jnp.float32)
    query_rot = rotate(query_rows.astype(jnp.float32).reshape(length, head_count, key_size), positions).astype(jnp.bfloat16)
    key_rot = (rotate(key_rows.astype(jnp.float32).reshape(length, head_count, key_size), positions) * key_size ** (-0.5)).astype(jnp.bfloat16)
    block_count = length // BLOCK
    query_blk = query_rot.reshape(block_count, BLOCK, head_count, key_size)
    key_blk = key_rot.reshape(block_count, BLOCK, head_count, key_size)
    value_blk = value_rows.reshape(block_count, BLOCK, head_count, value_size)
    inner, keep_fwd, keep_bwd, reach_fwd, reach_bwd = decay_tables(rate_fwd, rate_bwd, BLOCK)
    span_fwd = jnp.exp(rate_fwd * BLOCK)[:, None, None]
    span_bwd = jnp.exp(rate_bwd * BLOCK)[:, None, None]
    highest_precision = lax.Precision.HIGHEST

    def carry_step(keep_factor, decay_reach, span):

        def step(running_state, blocks):
            query_block_rows, key_block_rows, value_block_rows = blocks
            carried_state = jnp.einsum('zdf,dfe->zde', query_block_rows.astype(jnp.float32) * decay_reach.T[:, :, None], running_state, precision=highest_precision)
            state_update = jnp.einsum('tmu,tme->mue', key_block_rows.astype(jnp.float32) * keep_factor.T[:, :, None], value_block_rows.astype(jnp.float32), precision=highest_precision)
            return (span * running_state + state_update, carried_state)
        return step
    start_state = jnp.zeros((head_count, key_size, value_size), jnp.float32)
    blocks_all = (query_blk, key_blk, value_blk)
    _, carried_fwd = lax.scan(carry_step(keep_fwd, reach_fwd, span_fwd), start_state, blocks_all)
    _, carried_bwd = lax.scan(carry_step(keep_bwd, reach_bwd, span_bwd), start_state, blocks_all, reverse=True)

    def inside(blocks):
        query_block_rows, key_block_rows, value_block_rows = blocks
        scores = jnp.einsum('thk,shk->hts', query_block_rows.astype(jnp.float32), key_block_rows.astype(jnp.float32), precision=highest_precision)
        weights = (scores * inner).astype(jnp.bfloat16)
        return jnp.einsum('hts,shv->thv', weights.astype(jnp.float32), value_block_rows.astype(jnp.float32), precision=highest_precision)
    local_terms = lax.map(inside, blocks_all)
    combined = (local_terms + carried_fwd + carried_bwd).reshape(length, head_count, value_size)
    return head_gate(combined, gate_rows)

def rms_scale(rows_in, gain):
    widened = rows_in.astype(jnp.float32)
    return (widened * lax.rsqrt(lax.optimization_barrier(jnp.mean(widened * widened, -1, keepdims=True)) + NORM_EPSILON) * gain).astype(jnp.bfloat16)

def reference(stream, query_narrow, key_narrow, query_wide, key_wide, values, out_gate, out_weight, norm_gain, mlp_gate, mlp_up, mlp_down, log_decay):
    narrow_out = retention_group(query_narrow, key_narrow, values[:, 0], out_gate[:, 0], log_decay[0, 0], log_decay[1, 0])
    wide_out = retention_group(query_wide, key_wide, values[:, 1], out_gate[:, 1], log_decay[0, 1], log_decay[1, 1])

    def layer_rows(pieces):
        stream_rows, narrow_rows, wide_rows = pieces
        projection = jnp.dot(narrow_rows, out_weight[0], preferred_element_type=jnp.float32) + jnp.dot(wide_rows, out_weight[1], preferred_element_type=jnp.float32)
        middle = (stream_rows.astype(jnp.float32) + projection).astype(jnp.bfloat16)
        normed = rms_scale(middle, norm_gain)
        gate_act = jnp.dot(normed, mlp_gate, preferred_element_type=jnp.float32)
        up_act = jnp.dot(normed, mlp_up, preferred_element_type=jnp.float32)
        hidden = (jax.nn.silu(gate_act) * up_act).astype(jnp.bfloat16)
        down = jnp.dot(hidden, mlp_down, preferred_element_type=jnp.float32)
        return (middle.astype(jnp.float32) + 0.5 * down).astype(jnp.bfloat16)
    result = lax.map(layer_rows, (stream.reshape(N_SP, TOK_DEV, D), narrow_out.reshape(N_SP, TOK_DEV, -1), wide_out.reshape(N_SP, TOK_DEV, -1)))
    return result.reshape(TOKENS, D)
```

```python
import jax
import jax.numpy as jnp
from jax import lax
from jax.sharding import PartitionSpec as P

NORM_EPSILON = 1e-06
ROPE_BASE = 10000.0
BF = jnp.bfloat16
F32 = jnp.float32


def rope_tables(positions, key_size):
    half = key_size // 2
    frequencies = jnp.power(ROPE_BASE, -(jnp.arange(half, dtype=F32) / half))
    angles = positions[:, None] * frequencies[None, :]
    return jnp.cos(angles)[None], jnp.sin(angles)[None]


def rotate(rows, tables):
    cosine, sine = tables
    half = rows.shape[-1] // 2
    a, b = rows[..., :half], rows[..., half:]
    return jnp.concatenate([a * cosine - b * sine, a * sine + b * cosine], -1)


def heads_first(rows, heads):
    return rows.reshape(rows.shape[0], heads, -1).transpose(1, 0, 2)


def local_part(query_rows, key_rows, value_rows, rate_fwd, rate_bwd, positions):
    length = query_rows.shape[0]
    heads = rate_fwd.shape[0]
    key_size = query_rows.shape[1] // heads
    tables = rope_tables(positions, key_size)
    q = rotate(heads_first(query_rows, heads).astype(F32), tables).astype(BF)
    k = (rotate(heads_first(key_rows, heads).astype(F32), tables) * key_size ** (-0.5)).astype(BF)
    v = heads_first(value_rows, heads)
    step = jnp.arange(length, dtype=F32)
    k32 = k.astype(F32)
    k_fwd = (k32 * jnp.exp(rate_fwd[:, None] * (length - 1.0 - step)[None])[..., None]).astype(BF)
    k_bwd = (k32 * jnp.exp(rate_bwd[:, None] * step[None])[..., None]).astype(BF)
    keys = jnp.concatenate([k_fwd, k_bwd], -1)
    state = jnp.einsum("hsk,hsv->hkv", keys, v, preferred_element_type=F32).astype(BF)
    return q, k, v, state


def inside_part(q, k, v, rate_fwd, rate_bwd):
    length = q.shape[1]
    step = jnp.arange(length, dtype=F32)
    offset = (step[:, None] - step[None, :])[None]
    power = jnp.where(offset > 0, rate_fwd[:, None, None], -rate_bwd[:, None, None]) * offset
    weight = jnp.where(offset == 0, 2.0, jnp.exp(power))
    scores = jnp.einsum("htk,hsk->hts", q, k, preferred_element_type=F32)
    return jnp.einsum("hts,hsv->htv", (scores * weight).astype(BF), v, preferred_element_type=F32)


def finish(q, inside, enter, rate_fwd, rate_bwd, gate_rows):
    heads, length, _ = q.shape
    step = jnp.arange(length, dtype=F32)
    q32 = q.astype(F32)
    q_fwd = (q32 * jnp.exp(rate_fwd[:, None] * (step + 1.0)[None])[..., None]).astype(BF)
    q_bwd = (q32 * jnp.exp(rate_bwd[:, None] * (length - step)[None])[..., None]).astype(BF)
    both = jnp.concatenate([q_fwd, q_bwd], -1)
    ret = inside + jnp.einsum("htk,hkv->htv", both, enter, preferred_element_type=F32)
    centred = ret - jnp.mean(ret, -1, keepdims=True)
    variance = jnp.mean(centred * centred, -1, keepdims=True)
    scaled = centred * lax.rsqrt(variance + NORM_EPSILON)
    gated = jax.nn.silu(heads_first(gate_rows, heads).astype(F32)) * scaled
    return gated.astype(BF).transpose(1, 0, 2).reshape(length, -1)


def exchange_states(packed, rates, is_fwd, length):
    count, me = lax.axis_size("sp"), lax.axis_index("sp")
    rows, width = packed.shape
    share = rows // count
    got = lax.all_to_all(packed.reshape(count, share, width), "sp", 0, 0)
    rate = lax.dynamic_slice_in_dim(rates, me * share, share)
    fwd = lax.dynamic_slice_in_dim(is_fwd, me * share, share)
    index = jnp.arange(count, dtype=F32)
    gap = (index[:, None] - index[None, :])[:, :, None]
    gap = jnp.where(fwd[None, None, :] > 0, gap, -gap)
    factor = jnp.where(gap > 0, jnp.exp(rate * length * jnp.maximum(gap - 1.0, 0.0)), 0.0)
    got32 = got.astype(F32)
    entering = jnp.zeros((count, share, width), F32)
    for j in range(count):
        entering += factor[:, j, :, None] * got32[j][None]
    entering = entering.astype(BF)
    return lax.all_to_all(entering, "sp", 0, 0).reshape(rows, width)


def shift_tp(array, by):
    count = lax.axis_size("tp")
    return lax.ppermute(array, "tp", [((i + by) % count, i) for i in range(count)])


def from_all(array):
    return [array] + [shift_tp(array, by) for by in range(1, lax.axis_size("tp"))]


def in_order(pieces):
    count, me = len(pieces), lax.axis_index("tp")
    ordered = []
    for place in range(count):
        piece = pieces[0]
        for ahead in range(1, count):
            piece = jnp.where((me + ahead) % count == place, pieces[ahead], piece)
        ordered.append(piece)
    return jnp.concatenate(ordered, 0)


def body(
    stream,
    query_narrow,
    key_narrow,
    query_wide,
    key_wide,
    values,
    out_gate,
    out_weight,
    norm_gain,
    mlp_gate,
    mlp_up,
    mlp_down,
    log_decay,
):
    tp = lax.axis_index("tp")
    full_gate = lax.all_gather(mlp_gate, "sp", axis=0, tiled=True)
    full_up = lax.all_gather(mlp_up, "sp", axis=0, tiled=True)
    full_down = lax.all_gather(mlp_down, "sp", axis=1, tiled=True)
    weights = from_all(out_weight.reshape(-1, out_weight.shape[-1]))
    stream_rows = in_order(from_all(stream))

    length = query_narrow.shape[0]
    positions = (lax.axis_index("sp") * length + jnp.arange(length, dtype=jnp.int32)).astype(F32)
    queries, keys = (query_narrow, query_wide), (key_narrow, key_wide)
    parts, states, rates, is_fwd = [], [], [], []
    for g in range(2):
        fwd, bwd = log_decay[0, g], log_decay[1, g]
        q, k, v, state = local_part(queries[g], keys[g], values[:, g], fwd, bwd, positions)
        parts.append((q, k, v, fwd, bwd))
        states.append(state)
        heads, key_size = q.shape[0], q.shape[2]
        rates.append(jnp.repeat(jnp.stack([fwd, bwd], 1).reshape(-1), key_size))
        is_fwd.append(jnp.tile(jnp.repeat(jnp.array([1.0, 0.0], F32), key_size), heads))
    width = states[0].shape[-1]
    packed = jnp.concatenate([s.reshape(-1, width) for s in states], 0)
    entering = exchange_states(packed, jnp.concatenate(rates), jnp.concatenate(is_fwd), float(length))
    outs, at = [], 0
    for g in range(2):
        q, k, v, fwd, bwd = parts[g]
        size = states[g].shape[0] * states[g].shape[1]
        enter = entering[at : at + size].reshape(states[g].shape)
        at += size
        inside = inside_part(q, k, v, fwd, bwd)
        outs.append(finish(q, inside, enter, fwd, bwd, out_gate[:, g]))
    ys = from_all(jnp.concatenate(outs, 1))
    proj = jnp.dot(ys[0], weights[0], preferred_element_type=F32)
    for y, weight in zip(ys[1:], weights[1:]):
        proj += jnp.dot(y, weight, preferred_element_type=F32)
    middle = (stream_rows.astype(F32) + proj).astype(BF)
    wide = middle.astype(F32)
    normed = (
        wide * lax.rsqrt(jnp.mean(wide * wide, -1, keepdims=True) + NORM_EPSILON) * norm_gain
    ).astype(BF)
    gate_act = jnp.dot(normed, full_gate, preferred_element_type=F32)
    up_act = jnp.dot(normed, full_up, preferred_element_type=F32)
    hidden = (jax.nn.silu(gate_act) * up_act).astype(BF)
    rows, count = stream.shape[0], lax.axis_size("tp")
    down = 0.0
    for by in list(range(1, count)) + [0]:
        start = ((tp + by) % count) * rows
        part = jnp.dot(
            lax.dynamic_slice_in_dim(hidden, start, rows), full_down, preferred_element_type=F32
        )
        down += shift_tp(part.astype(BF), count - by).astype(F32) if by else part
    middle_mine = lax.dynamic_slice_in_dim(middle, tp * rows, rows)
    return (middle_mine.astype(F32) + 0.5 * down).astype(BF)


def solution(mesh):
    return jax.shard_map(
        body,
        mesh=mesh,
        in_specs=(
            P(("sp", "tp"), None),
            P("sp", "tp"),
            P("sp", "tp"),
            P("sp", "tp"),
            P("sp", "tp"),
            P("sp", None, "tp"),
            P("sp", None, "tp"),
            P(None, "tp", None),
            P(),
            P("sp", "tp"),
            P("sp", "tp"),
            P("tp", "sp"),
            P(None, None, "tp"),
        ),
        out_specs=P(("sp", "tp"), None),
        check_vma=False,
    )
```

```python
import jax
import jax.numpy as jnp
from jax import lax
from jax.sharding import PartitionSpec as P

NORM_EPSILON = 1e-06
ROPE_BASE = 10000.0
BF = jnp.bfloat16
F32 = jnp.float32
CORE, SHARE = 1, 2


def rope_tables(positions, key_size):
    half = key_size // 2
    frequencies = jnp.power(ROPE_BASE, -(jnp.arange(half, dtype=F32) / half))
    angles = positions[:, None] * frequencies[None, :]
    return jnp.cos(angles)[None], jnp.sin(angles)[None]


def rotate(rows, tables):
    cosine, sine = tables
    half = rows.shape[-1] // 2
    a, b = rows[..., :half], rows[..., half:]
    return jnp.concatenate([a * cosine - b * sine, a * sine + b * cosine], -1)


def heads_first(rows, heads):
    return rows.reshape(rows.shape[0], heads, -1).transpose(1, 0, 2)


def local_part(query_rows, key_rows, value_rows, rate_fwd, rate_bwd, positions):
    length = query_rows.shape[0]
    heads = rate_fwd.shape[0]
    key_size = query_rows.shape[1] // heads
    tables = rope_tables(positions, key_size)
    q = rotate(heads_first(query_rows, heads).astype(F32), tables).astype(BF)
    k = (rotate(heads_first(key_rows, heads).astype(F32), tables) * key_size ** (-0.5)).astype(BF)
    v = heads_first(value_rows, heads)
    step = jnp.arange(length, dtype=F32)
    k32 = k.astype(F32)
    k_fwd = (k32 * jnp.exp(rate_fwd[:, None] * (length - 1.0 - step)[None])[..., None]).astype(BF)
    k_bwd = (k32 * jnp.exp(rate_bwd[:, None] * step[None])[..., None]).astype(BF)
    keys = jnp.concatenate([k_fwd, k_bwd], -1)
    state = jnp.einsum("hsk,hsv->hkv", keys, v, preferred_element_type=F32).astype(BF)
    return q, k, v, state


def inside_part(q, k, v, rate_fwd, rate_bwd):
    length = q.shape[1]
    step = jnp.arange(length, dtype=F32)
    offset = (step[:, None] - step[None, :])[None]
    power = jnp.where(offset > 0, rate_fwd[:, None, None], -rate_bwd[:, None, None]) * offset
    weight = jnp.where(offset == 0, 2.0, jnp.exp(power))
    scores = jnp.einsum("htk,hsk->hts", q, k, preferred_element_type=F32)
    return jnp.einsum("hts,hsv->htv", (scores * weight).astype(BF), v, preferred_element_type=F32)


def finish(q, inside, enter, rate_fwd, rate_bwd, gate_rows):
    heads, length, _ = q.shape
    step = jnp.arange(length, dtype=F32)
    q32 = q.astype(F32)
    q_fwd = (q32 * jnp.exp(rate_fwd[:, None] * (step + 1.0)[None])[..., None]).astype(BF)
    q_bwd = (q32 * jnp.exp(rate_bwd[:, None] * (length - step)[None])[..., None]).astype(BF)
    both = jnp.concatenate([q_fwd, q_bwd], -1)
    ret = inside + jnp.einsum("htk,hkv->htv", both, enter, preferred_element_type=F32)
    centred = ret - jnp.mean(ret, -1, keepdims=True)
    variance = jnp.mean(centred * centred, -1, keepdims=True)
    scaled = centred * lax.rsqrt(variance + NORM_EPSILON)
    gated = jax.nn.silu(heads_first(gate_rows, heads).astype(F32)) * scaled
    return gated.astype(BF).transpose(1, 0, 2).reshape(length, -1)


def exchange_states(packed, rates, is_fwd, length):
    count, me = lax.axis_size("sp"), lax.axis_index("sp")
    rows, width = packed.shape
    share = rows // count
    got = lax.all_to_all(packed.reshape(count, share, width), "sp", 0, 0)
    rate = lax.dynamic_slice_in_dim(rates, me * share, share)
    fwd = lax.dynamic_slice_in_dim(is_fwd, me * share, share)
    index = jnp.arange(count, dtype=F32)
    gap = (index[:, None] - index[None, :])[:, :, None]
    gap = jnp.where(fwd[None, None, :] > 0, gap, -gap)
    factor = jnp.where(gap > 0, jnp.exp(rate * length * jnp.maximum(gap - 1.0, 0.0)), 0.0)
    got32 = got.astype(F32)
    entering = jnp.zeros((count, share, width), F32)
    for j in range(count):
        entering += factor[:, j, :, None] * got32[j][None]
    entering = entering.astype(BF)
    return lax.all_to_all(entering, "sp", 0, 0).reshape(rows, width)


def fetch(array, flip, ahead):
    n_sp, n_tp = lax.axis_size("sp"), lax.axis_size("tp")
    pairs = [
        ((i ^ flip) * n_tp + (j + ahead) % n_tp, i * n_tp + j)
        for i in range(n_sp)
        for j in range(n_tp)
    ]
    return lax.ppermute(array, ("sp", "tp"), pairs)


def flip_sp(array, flip):
    n_sp = lax.axis_size("sp")
    return lax.ppermute(array, "sp", [(i, i ^ flip) for i in range(n_sp)])


def far_bits():
    bits, bit = [], lax.axis_size("sp") // 2
    while bit > SHARE:
        bits.append(bit)
        bit //= 2
    return bits


def gather_weight(weight, cut_axis, join_axis):
    me = lax.axis_index("sp")
    upper = (me // SHARE) % 2 == 1
    low, high = jnp.split(weight, 2, axis=cut_axis)
    keep, send = jnp.where(upper, high, low), jnp.where(upper, low, high)
    got = flip_sp(send, SHARE)
    pair = [jnp.where(upper, got, keep), jnp.where(upper, keep, got)]
    pieces = [jnp.concatenate(pair, join_axis)]
    for bit in far_bits():
        pieces = pieces + [flip_sp(piece, bit) for piece in pieces]
    pieces = pieces + [flip_sp(piece, CORE) for piece in pieces]
    return jnp.concatenate(pieces, join_axis)


def to_flipped(rows):
    me, bits = lax.axis_index("sp"), far_bits()
    n = len(bits)
    split = rows.reshape([rows.shape[0]] + [2] * n + [2, 2, -1])
    for axis, bit in list(enumerate(bits)) + [(n + 1, CORE)]:
        split = jnp.where((me // bit) % 2 == 1, jnp.flip(split, axis + 1), split)
    split = split.transpose([0, n + 2] + list(range(n, 0, -1)) + [n + 1, n + 3])
    return split.reshape(rows.shape)


def from_flipped(rows):
    me, bits = lax.axis_index("sp"), far_bits()
    n = len(bits)
    split = rows.reshape([rows.shape[0], 2] + [2] * n + [2, -1])
    split = split.transpose([0] + list(range(n + 1, 1, -1)) + [n + 2, 1, n + 3])
    for axis, bit in list(enumerate(bits)) + [(n + 1, CORE)]:
        split = jnp.where((me // bit) % 2 == 1, jnp.flip(split, axis + 1), split)
    return split.reshape(rows.shape)


def from_all(array, flip=0):
    count = lax.axis_size("tp")
    return [fetch(array, flip, by) if flip or by else array for by in range(count)]


def in_order(pieces):
    count, me = len(pieces), lax.axis_index("tp")
    ordered = []
    for place in range(count):
        piece = pieces[0]
        for ahead in range(1, count):
            piece = jnp.where((me + ahead) % count == place, pieces[ahead], piece)
        ordered.append(piece)
    return jnp.concatenate(ordered, 0)


def body(
    stream,
    query_narrow,
    key_narrow,
    query_wide,
    key_wide,
    values,
    out_gate,
    out_weight,
    norm_gain,
    mlp_gate,
    mlp_up,
    mlp_down,
    log_decay,
):
    tp = lax.axis_index("tp")
    full_gate = gather_weight(mlp_gate, 1, 0)
    full_up = gather_weight(mlp_up, 1, 0)
    full_down = gather_weight(mlp_down, 0, 1)
    weights = from_all(out_weight.reshape(-1, out_weight.shape[-1]))
    stream_rows = in_order(from_all(stream))
    stream_else = flip_sp(stream_rows, SHARE)

    length = query_narrow.shape[0]
    positions = (lax.axis_index("sp") * length + jnp.arange(length, dtype=jnp.int32)).astype(F32)
    queries, keys = (query_narrow, query_wide), (key_narrow, key_wide)
    parts, states, rates, is_fwd = [], [], [], []
    for g in range(2):
        fwd, bwd = log_decay[0, g], log_decay[1, g]
        q, k, v, state = local_part(queries[g], keys[g], values[:, g], fwd, bwd, positions)
        parts.append((q, k, v, fwd, bwd))
        states.append(state)
        heads, key_size = q.shape[0], q.shape[2]
        rates.append(jnp.repeat(jnp.stack([fwd, bwd], 1).reshape(-1), key_size))
        is_fwd.append(jnp.tile(jnp.repeat(jnp.array([1.0, 0.0], F32), key_size), heads))
    width = states[0].shape[-1]
    packed = jnp.concatenate([s.reshape(-1, width) for s in states], 0)
    entering = exchange_states(packed, jnp.concatenate(rates), jnp.concatenate(is_fwd), float(length))
    outs, at = [], 0
    for g in range(2):
        q, k, v, fwd, bwd = parts[g]
        size = states[g].shape[0] * states[g].shape[1]
        enter = entering[at : at + size].reshape(states[g].shape)
        at += size
        inside = inside_part(q, k, v, fwd, bwd)
        outs.append(finish(q, inside, enter, fwd, bwd, out_gate[:, g]))
    mine = jnp.concatenate(outs, 1)
    rows, count = stream.shape[0], lax.axis_size("tp")
    both = [from_all(mine), from_all(mine, SHARE)]
    middles, downs = {}, []
    for flip, ys, residual in ((0, both[0], stream_rows), (SHARE, both[1], stream_else)):
        proj = jnp.dot(ys[0], weights[0], preferred_element_type=F32)
        for y, weight in zip(ys[1:], weights[1:]):
            proj += jnp.dot(y, weight, preferred_element_type=F32)
        middle = (residual.astype(F32) + proj).astype(BF)
        wide = middle.astype(F32)
        normed = (
            wide * lax.rsqrt(jnp.mean(wide * wide, -1, keepdims=True) + NORM_EPSILON) * norm_gain
        ).astype(BF)
        middles[flip] = (middle, to_flipped(normed))
    for flip in (SHARE, 0):
        normed = middles[flip][1]
        gate_act = jnp.dot(normed, full_gate, preferred_element_type=F32)
        up_act = jnp.dot(normed, full_up, preferred_element_type=F32)
        hidden = (jax.nn.silu(gate_act) * up_act).astype(BF)
        for by in list(range(1, count)) + [0]:
            start = ((tp + by) % count) * rows
            part = jnp.dot(
                lax.dynamic_slice_in_dim(hidden, start, rows), full_down, preferred_element_type=F32
            )
            if flip or by:
                part = fetch(part.astype(BF), flip, count - by).astype(F32)
            downs.append(part)
    down = from_flipped(sum(downs[1:], downs[0]))
    middle_mine = lax.dynamic_slice_in_dim(middles[0][0], tp * rows, rows)
    return (middle_mine.astype(F32) + 0.5 * down).astype(BF)


def solution(mesh):
    return jax.shard_map(
        body,
        mesh=mesh,
        in_specs=(
            P(("sp", "tp"), None),
            P("sp", "tp"),
            P("sp", "tp"),
            P("sp", "tp"),
            P("sp", "tp"),
            P("sp", None, "tp"),
            P("sp", None, "tp"),
            P(None, "tp", None),
            P(),
            P("sp", "tp"),
            P("sp", "tp"),
            P("tp", "sp"),
            P(None, None, "tp"),
        ),
        out_specs=P(("sp", "tp"), None),
        check_vma=False,
    )
```

```python
import jax
import jax.numpy as jnp
from jax import lax
from jax.sharding import PartitionSpec as P

NORM_EPSILON = 1e-06
ROPE_BASE = 10000.0
BF = jnp.bfloat16
F32 = jnp.float32
SHARE = 2


def rope_tables(positions, key_size):
    half = key_size // 2
    frequencies = jnp.power(ROPE_BASE, -(jnp.arange(half, dtype=F32) / half))
    angles = positions[:, None] * frequencies[None, :]
    return jnp.cos(angles)[None], jnp.sin(angles)[None]


def rotate(rows, tables):
    cosine, sine = tables
    half = rows.shape[-1] // 2
    a, b = rows[..., :half], rows[..., half:]
    return jnp.concatenate([a * cosine - b * sine, a * sine + b * cosine], -1)


def heads_first(rows, heads):
    return rows.reshape(rows.shape[0], heads, -1).transpose(1, 0, 2)


def local_part(query_rows, key_rows, value_rows, rate_fwd, rate_bwd, positions):
    length = query_rows.shape[0]
    heads = rate_fwd.shape[0]
    key_size = query_rows.shape[1] // heads
    tables = rope_tables(positions, key_size)
    q = rotate(heads_first(query_rows, heads).astype(F32), tables).astype(BF)
    k = (rotate(heads_first(key_rows, heads).astype(F32), tables) * key_size ** (-0.5)).astype(BF)
    v = heads_first(value_rows, heads)
    step = jnp.arange(length, dtype=F32)
    k32 = k.astype(F32)
    k_fwd = (k32 * jnp.exp(rate_fwd[:, None] * (length - 1.0 - step)[None])[..., None]).astype(BF)
    k_bwd = (k32 * jnp.exp(rate_bwd[:, None] * step[None])[..., None]).astype(BF)
    keys = jnp.concatenate([k_fwd, k_bwd], -1)
    state = jnp.einsum("hsk,hsv->hkv", keys, v, preferred_element_type=F32).astype(BF)
    return q, k, v, state


def inside_part(q, k, v, rate_fwd, rate_bwd):
    length = q.shape[1]
    step = jnp.arange(length, dtype=F32)
    offset = (step[:, None] - step[None, :])[None]
    power = jnp.where(offset > 0, rate_fwd[:, None, None], -rate_bwd[:, None, None]) * offset
    weight = jnp.where(offset == 0, 2.0, jnp.exp(power))
    scores = jnp.einsum("htk,hsk->hts", q, k, preferred_element_type=F32)
    return jnp.einsum("hts,hsv->htv", (scores * weight).astype(BF), v, preferred_element_type=F32)


def finish(q, inside, enter, rate_fwd, rate_bwd, gate_rows):
    heads, length, _ = q.shape
    step = jnp.arange(length, dtype=F32)
    q32 = q.astype(F32)
    q_fwd = (q32 * jnp.exp(rate_fwd[:, None] * (step + 1.0)[None])[..., None]).astype(BF)
    q_bwd = (q32 * jnp.exp(rate_bwd[:, None] * (length - step)[None])[..., None]).astype(BF)
    both = jnp.concatenate([q_fwd, q_bwd], -1)
    ret = inside + jnp.einsum("htk,hkv->htv", both, enter, preferred_element_type=F32)
    centred = ret - jnp.mean(ret, -1, keepdims=True)
    variance = jnp.mean(centred * centred, -1, keepdims=True)
    scaled = centred * lax.rsqrt(variance + NORM_EPSILON)
    gated = jax.nn.silu(heads_first(gate_rows, heads).astype(F32)) * scaled
    return gated.astype(BF).transpose(1, 0, 2).reshape(length, -1)


def exchange_states(packed, rates, is_fwd, length):
    count, me = lax.axis_size("sp"), lax.axis_index("sp")
    rows, width = packed.shape
    share = rows // count
    got = lax.all_to_all(packed.reshape(count, share, width), "sp", 0, 0)
    rate = lax.dynamic_slice_in_dim(rates, me * share, share)
    fwd = lax.dynamic_slice_in_dim(is_fwd, me * share, share)
    index = jnp.arange(count, dtype=F32)
    gap = (index[:, None] - index[None, :])[:, :, None]
    gap = jnp.where(fwd[None, None, :] > 0, gap, -gap)
    factor = jnp.where(gap > 0, jnp.exp(rate * length * jnp.maximum(gap - 1.0, 0.0)), 0.0)
    got32 = got.astype(F32)
    entering = jnp.zeros((count, share, width), F32)
    for j in range(count):
        entering += factor[:, j, :, None] * got32[j][None]
    entering = entering.astype(BF)
    return lax.all_to_all(entering, "sp", 0, 0).reshape(rows, width)


def fetch(array, flip, ahead):
    n_sp, n_tp = lax.axis_size("sp"), lax.axis_size("tp")
    pairs = [
        ((i ^ flip) * n_tp + (j + ahead) % n_tp, i * n_tp + j)
        for i in range(n_sp)
        for j in range(n_tp)
    ]
    return lax.ppermute(array, ("sp", "tp"), pairs)


def flip_sp(array, flip):
    n_sp = lax.axis_size("sp")
    return lax.ppermute(array, "sp", [(i, i ^ flip) for i in range(n_sp)])


def halve_weight(weight, cut_axis, join_axis):
    me, n_sp = lax.axis_index("sp"), lax.axis_size("sp")
    core, upper = me % 2 == 1, (me // SHARE) % 2 == 1
    low, high = jnp.split(weight, 2, axis=cut_axis)
    same, cross = jnp.where(core, high, low), jnp.where(core, low, high)
    base = [i - i % 4 for i in range(n_sp)]
    x_of, c_of = [(i // 2) % 2 for i in range(n_sp)], [i % 2 for i in range(n_sp)]
    to_same = [(i, base[i] + 2 * c_of[i] + x_of[i]) for i in range(n_sp)]
    to_cross = [(i, base[i] + 2 * (1 - c_of[i]) + x_of[i]) for i in range(n_sp)]
    first = lax.ppermute(same, "sp", to_same)
    second = lax.ppermute(cross, "sp", to_cross)
    pair = [jnp.where(upper, second, first), jnp.where(upper, first, second)]
    return jnp.concatenate(pair, join_axis)


def gather_weight(pair, axis):
    count = lax.axis_size("sp")
    groups = [[i for i in range(count) if (i // SHARE) % 2 == half] for half in range(2)]
    return lax.all_gather(pair, "sp", axis=axis, tiled=True, axis_index_groups=groups)


def from_all(array, flip=0):
    count = lax.axis_size("tp")
    return [fetch(array, flip, by) if flip or by else array for by in range(count)]


def in_order(pieces):
    count, me = len(pieces), lax.axis_index("tp")
    ordered = []
    for place in range(count):
        piece = pieces[0]
        for ahead in range(1, count):
            piece = jnp.where((me + ahead) % count == place, pieces[ahead], piece)
        ordered.append(piece)
    return jnp.concatenate(ordered, 0)


def body(
    stream,
    query_narrow,
    key_narrow,
    query_wide,
    key_wide,
    values,
    out_gate,
    out_weight,
    norm_gain,
    mlp_gate,
    mlp_up,
    mlp_down,
    log_decay,
):
    tp = lax.axis_index("tp")
    halves = (
        halve_weight(mlp_gate, 1, 0),
        halve_weight(mlp_up, 1, 0),
        halve_weight(mlp_down, 0, 1),
    )
    halves, query_wide, query_narrow, key_wide, key_narrow, values = lax.optimization_barrier(
        (halves, query_wide, query_narrow, key_wide, key_narrow, values)
    )
    full_gate = gather_weight(halves[0], 0)
    full_up = gather_weight(halves[1], 0)
    full_down = gather_weight(halves[2], 1)
    weights = from_all(out_weight.reshape(-1, out_weight.shape[-1]))
    stream_rows = in_order(from_all(stream))
    stream_else = flip_sp(stream_rows, SHARE)

    length = query_narrow.shape[0]
    positions = (lax.axis_index("sp") * length + jnp.arange(length, dtype=jnp.int32)).astype(F32)
    queries, keys = (query_narrow, query_wide), (key_narrow, key_wide)
    parts, states, rates, is_fwd = [], [], [], []
    for g in range(2):
        fwd, bwd = log_decay[0, g], log_decay[1, g]
        q, k, v, state = local_part(queries[g], keys[g], values[:, g], fwd, bwd, positions)
        parts.append((q, k, v, fwd, bwd))
        states.append(state)
        heads, key_size = q.shape[0], q.shape[2]
        rates.append(jnp.repeat(jnp.stack([fwd, bwd], 1).reshape(-1), key_size))
        is_fwd.append(jnp.tile(jnp.repeat(jnp.array([1.0, 0.0], F32), key_size), heads))
    width = states[0].shape[-1]
    packed = jnp.concatenate([s.reshape(-1, width) for s in states], 0)
    entering = exchange_states(packed, jnp.concatenate(rates), jnp.concatenate(is_fwd), float(length))
    outs, at = [], 0
    for g in range(2):
        q, k, v, fwd, bwd = parts[g]
        size = states[g].shape[0] * states[g].shape[1]
        enter = entering[at : at + size].reshape(states[g].shape)
        at += size
        inside = inside_part(q, k, v, fwd, bwd)
        outs.append(finish(q, inside, enter, fwd, bwd, out_gate[:, g]))
    mine = jnp.concatenate(outs, 1)
    rows, count = stream.shape[0], lax.axis_size("tp")
    both = [from_all(mine), from_all(mine, SHARE)]
    middles, downs = {}, []
    for flip, ys, residual in ((0, both[0], stream_rows), (SHARE, both[1], stream_else)):
        proj = jnp.dot(ys[0], weights[0], preferred_element_type=F32)
        for y, weight in zip(ys[1:], weights[1:]):
            proj += jnp.dot(y, weight, preferred_element_type=F32)
        middle = (residual.astype(F32) + proj).astype(BF)
        wide = middle.astype(F32)
        normed = (
            wide * lax.rsqrt(jnp.mean(wide * wide, -1, keepdims=True) + NORM_EPSILON) * norm_gain
        ).astype(BF)
        middles[flip] = (middle, normed)
    for flip in (SHARE, 0):
        normed = middles[flip][1]
        gate_act = jnp.dot(normed, full_gate, preferred_element_type=F32)
        up_act = jnp.dot(normed, full_up, preferred_element_type=F32)
        hidden = (jax.nn.silu(gate_act) * up_act).astype(BF)
        for by in list(range(1, count)) + [0]:
            start = ((tp + by) % count) * rows
            part = jnp.dot(
                lax.dynamic_slice_in_dim(hidden, start, rows), full_down, preferred_element_type=F32
            )
            if flip or by:
                part = fetch(part.astype(BF), flip, count - by).astype(F32)
            downs.append(part)
    down = sum(downs[1:], downs[0])
    middle_mine = lax.dynamic_slice_in_dim(middles[0][0], tp * rows, rows)
    return (middle_mine.astype(F32) + 0.5 * down).astype(BF)


def solution(mesh):
    return jax.shard_map(
        body,
        mesh=mesh,
        in_specs=(
            P(("sp", "tp"), None),
            P("sp", "tp"),
            P("sp", "tp"),
            P("sp", "tp"),
            P("sp", "tp"),
            P("sp", None, "tp"),
            P("sp", None, "tp"),
            P(None, "tp", None),
            P(),
            P("sp", "tp"),
            P("sp", "tp"),
            P("tp", "sp"),
            P(None, None, "tp"),
        ),
        out_specs=P(("sp", "tp"), None),
        check_vma=False,
    )
```
